32 devices in a mesh: sp: 8 (over z, x), tp: 4 (over y, core).
Axes of the slice: x: 2, y: 2, z: 4, core: 2. Of those that a mesh axis runs over, the one named last changes fastest.
Arguments:
- query_rows: bfloat16 [2048, 2048], P('sp', 'tp'), may hold values from -6 to 6
- key_rows: bfloat16 [2048, 2048], P('sp', 'tp'), may hold values from -6 to 6
- value_rows: bfloat16 [2048, 2048], P('sp', 'tp'), may hold values from -6 to 6
- gate_rows: bfloat16 [2048, 2048], P('sp', 'tp'), may hold values from -6 to 6
- log_decay: float32 [2048, 16], P('sp', 'tp'), may hold values from -1 to 0
- head_gain: float32 [2048], P('tp'), may hold values from 0.1 to 1.9
- out_weight: bfloat16 [2048, 2048], P('tp'), may hold values from -0.125 to 0.125
- residual: bfloat16 [2048, 2048], P(('sp', 'tp')), may hold values from -6 to 6
- ffn_gain: float32 [2048], replicated, may hold values from 0.1 to 1.9
- gate_weight: bfloat16 [8, 2048, 2048], P('sp', None, 'tp'), may hold values from -0.375 to 0.375
- up_weight: bfloat16 [8, 2048, 2048], P('sp', None, 'tp'), may hold values from -0.375 to 0.375
- down_weight: bfloat16 [8, 2048, 2048], P('sp', 'tp'), may hold values from -0.01953125 to 0.01953125
- routes: int32 [2048, 4], P('sp'), may hold values from 0 to 7, all different within a row; in each aligned block of 64 rows (0 to 63, 64 to 127, ...) at most 48 rows name the same one
- route_weights: float32 [2048, 4], P(('sp', 'tp')), may hold values from 0.05 to 1
Outputs:
- layer_out: bfloat16 [2048, 2048], P(('sp', 'tp'))
The draws below stay inside these ranges and needn't reach their ends.
Inputs may be any that keep to these rules, and one draw needn't show every extreme that they name: `routes`: each row names 4 different experts. In each aligned block of 64 rows no expert is named by more than 48 rows, and in some block some expert is named by exactly 48 rows.
All inputs are finite; a program needn't handle non-finite values.
Results may differ from the reference program's by a relative error of at most 0.014.
Values may be sent and summed in bfloat16 or wider, within the bound.
A program may use at most 128 MiB of HBM per device.

```python
import math
from functools import partial
import jax
import jax.numpy as jnp
import numpy as np
from jax import lax

D = 2048
HEAD_TOTAL = 16
HEAD_DIM = 128
FF = 2048
TOPK = 4
BLOCK = 128
TOK_DEV = 256
RET_WIDTH = 2048
EXPERTS = 8
TOKEN_TOTAL = 2048
ROWS_DEV = 64
CAP = 48
N_TP = 4


def draw_log_decay(key, part):
    split_random_keys = jax.random.split(jax.random.fold_in(key, 17), 7)
    fast_share = 0.5
    is_fast = jax.random.uniform(split_random_keys[0], (HEAD_TOTAL,), jnp.float32) < fast_share
    fast_rate = jnp.exp(jax.random.uniform(split_random_keys[1], (HEAD_TOTAL,), jnp.float32, math.log(1.0 / 15.0), math.log(1.0 / 8.0)))
    slow_rate = jnp.exp(jax.random.uniform(split_random_keys[2], (HEAD_TOTAL,), jnp.float32, math.log(0.05), math.log(0.25))) / TOKEN_TOTAL
    baseline_rate = jnp.where(is_fast, fast_rate, slow_rate)
    span_count = TOKEN_TOTAL // TOK_DEV
    extent_factor = jnp.exp(jax.random.uniform(split_random_keys[3], (span_count, HEAD_TOTAL), jnp.float32, -math.log(2.0), math.log(2.0)))
    extent_factor = jnp.repeat(extent_factor, TOK_DEV, axis=0)
    coarse_factor = jax.random.uniform(split_random_keys[4], (TOKEN_TOTAL, HEAD_TOTAL), jnp.float32, 0.5, 1.5)
    spike_position = jax.random.randint(split_random_keys[5], (3,), 0, TOKEN_TOTAL)
    spike_flags = jnp.zeros((TOKEN_TOTAL,), jnp.float32).at[spike_position].set(1.0)
    spike_penalty = jnp.log(jax.random.uniform(split_random_keys[6], (HEAD_TOTAL,), jnp.float32, 0.6, 0.8))
    return (-baseline_rate[None, :] * extent_factor * coarse_factor + spike_flags[:, None] * spike_penalty[None, :]).astype(jnp.float32)


def steps_of(rng, extent, shards, low, high):
    def one(dim, shards_of):
        heights = jax.random.uniform(jax.random.fold_in(jax.random.fold_in(rng, 6), dim), (shards_of,), jnp.float32, low / len(shards), high / len(shards))
        return jnp.repeat(jnp.exp(heights), extent[dim] // shards_of).reshape((-1,) + (1,) * (len(extent) - dim - 1))

    gain = one(*shards[0])
    for cut in shards[1:]:
        gain = gain * one(*cut)
    return gain


def deal_out(key, own, number, rows, amount, top, limit, lean):
    sequence = jax.random.permutation(key, amount)
    crowded, common = shares(amount, rows * top, limit, lean, True), shares(amount, rows * top, limit, lean, False)
    places = jnp.arange(amount)

    def named(lengths, rotation):
        used = int((lengths > 0).sum())
        fixed = max(1, used // 4)
        moved = fixed + (places - fixed + rotation * (used - fixed)) % max(1, amount - fixed)
        return jnp.zeros((amount,), jnp.int32).at[sequence[jnp.where(places < fixed, places, moved)]].set(jnp.asarray(lengths, jnp.int32))

    lengths = jnp.where(number % 4 == 0, named(crowded, number // 4), named(common, number - number // 4 - 1))
    mixed = jax.random.permutation(jax.random.fold_in(own, 3), amount)
    giver, receiver = mixed[0:amount // 2 * 2:2], mixed[1:amount // 2 * 2:2]
    margin = jnp.minimum(lengths[giver] - 1, limit - lengths[receiver]) // 2
    margin = jnp.where((giver == sequence[0]) | (receiver == sequence[0]) | (lengths[receiver] == 0), 0, jnp.maximum(margin, 0))
    moved = jax.random.randint(jax.random.fold_in(own, 4), (amount // 2,), 0, 1 << 20) % (margin + 1)
    lengths = lengths.at[giver].add(-moved).at[receiver].add(moved)
    members = jnp.searchsorted(jnp.cumsum(lengths), jnp.arange(rows * top), side="right").astype(jnp.int32)
    grid = members.reshape(top, rows).T
    grid = grid[jax.random.permutation(jax.random.fold_in(own, 1), rows)]
    rotation = jax.random.randint(jax.random.fold_in(own, 2), (rows, 1), 0, top)
    return jnp.take_along_axis(grid, (jnp.arange(top)[None, :] + rotation) % top, axis=1)


def shares(number_of, total, limit, skew, full):
    weights = [(1 << 20) // math.isqrt(rank ** skew) + 1 for rank in range(1, number_of + 1)]
    largest = limit if full else min(limit, max(-(-total // number_of), total * weights[0] // sum(weights)))
    least = 1 if total - largest >= number_of - 1 else 0
    holding, rest = [largest] + [least] * (number_of - 1), total - largest - least * (number_of - 1)
    while rest > 0:
        candidates = [i for i in range(1, number_of) if holding[i] < largest] or [i for i in range(1, number_of) if holding[i] < limit]
        whole, left = sum([weights[i] for i in candidates]), rest
        for i in candidates:
            addition = min(limit - holding[i], max(1, left * weights[i] // whole), rest)
            holding[i] = holding[i] + addition
            rest = rest - addition
    return np.array(holding)


def scatter_about(own_key, shape, scale, most, cuts=(), kind=jnp.bfloat16):
    entries = jax.random.normal(own_key, shape, jnp.float32) * scale
    if len(cuts) > 0:
        entries = steps_of(own_key, shape, cuts, -0.22, 0.18) * entries
    return jnp.clip(entries, min=-most, max=most).astype(kind)


def setup_inputs(seed: int = 0) -> dict:
    key_list = jax.random.split(jax.random.key(seed), 15)
    query_rows = scatter_about(key_list[0], (TOKEN_TOTAL, RET_WIDTH), 1.0, 6.0, ((0, 8), (1, 4)))
    key_rows = scatter_about(key_list[1], (TOKEN_TOTAL, RET_WIDTH), 1.0, 6.0, ((0, 8), (1, 4)))
    value_rows = scatter_about(key_list[2], (TOKEN_TOTAL, RET_WIDTH), 1.0, 6.0, ((0, 8), (1, 4)))
    gate_rows = scatter_about(key_list[3], (TOKEN_TOTAL, RET_WIDTH), 1.0, 6.0, ((0, 8), (1, 4)))
    log_decay = draw_log_decay(jax.random.fold_in(key_list[14], 71), 0)
    head_gain = jnp.clip(1.0 + 0.18 * jax.random.normal(key_list[5], (RET_WIDTH,), jnp.float32), 0.1, 1.9)
    out_weight = scatter_about(key_list[6], (RET_WIDTH, D), RET_WIDTH ** -0.5, 0.125, ((0, 4),))
    residual = scatter_about(key_list[7], (TOKEN_TOTAL, D), 1.0, 6.0, ((0, 32),))
    ffn_gain = jnp.clip(1.0 + 0.18 * jax.random.normal(key_list[8], (D,), jnp.float32), 0.1, 1.9)
    gate_weight = scatter_about(key_list[9], (EXPERTS, D, FF), (D // 9) ** -0.5, 0.375, ((0, 8), (2, 4)))
    up_weight = scatter_about(key_list[10], (EXPERTS, D, FF), (D // 9) ** -0.5, 0.375, ((0, 8), (2, 4)))
    down_weight = scatter_about(key_list[11], (EXPERTS, FF, D), (FF * 44) ** -0.5, 0.01953125, ((0, 8), (1, 4)))
    routes_keys = jax.random.split(jax.random.fold_in(key_list[12], 1), TOKEN_TOTAL // ROWS_DEV)
    routes_turns = jax.random.permutation(jax.random.fold_in(key_list[12], 3), TOKEN_TOTAL // ROWS_DEV)
    routes = jax.vmap(lambda own, number: deal_out(jax.random.fold_in(key_list[12], 2), own, number, ROWS_DEV, EXPERTS, TOPK, CAP, 1))(routes_keys, routes_turns).reshape((TOKEN_TOTAL, TOPK))
    route_weights = jnp.clip(jnp.exp(math.log(1.0) - 2.9957323 * jax.random.uniform(key_list[13], (TOKEN_TOTAL, TOPK), jnp.float32) ** steps_of(key_list[13], (TOKEN_TOTAL, TOPK), ((0, 32),), -0.2, 0.2)), 0.05, 1.0)
    return dict(query_rows=query_rows, key_rows=key_rows, value_rows=value_rows, gate_rows=gate_rows, log_decay=log_decay, head_gain=head_gain, out_weight=out_weight, residual=residual, ffn_gain=ffn_gain, gate_weight=gate_weight, up_weight=up_weight, down_weight=down_weight, routes=routes, route_weights=route_weights)


highest = lax.Precision.HIGHEST
rope_base = 10000.0
group_eps = 1e-05
square_eps = 1e-06
clamp_limit = 7.0
swish_alpha = 1.702

def rotary_angles(positions, head_dim):
    half_dim = head_dim // 2
    inverse = rope_base ** (-jnp.arange(half_dim, dtype=jnp.float32) / half_dim)
    return positions[:, None] * inverse[None, :]

def rotate(values, angles):
    half_dim = values.shape[-1] // 2
    cosine = jnp.cos(angles)[:, None, :]
    sine_table = jnp.sin(angles)[:, None, :]
    first_half = values[..., :half_dim]
    second_half = values[..., half_dim:]
    return jnp.concatenate([first_half * cosine - second_half * sine_table, second_half * cosine + first_half * sine_table], axis=-1)

def block_pass(carry_state, queries, keys_rot, values, log_step):
    length = queries.shape[0]
    cumulative = jnp.cumsum(log_step, axis=0)
    gap_matrix = cumulative[:, None, :] - cumulative[None, :, :]
    causal = jnp.arange(length, dtype=jnp.int32)[:, None] >= jnp.arange(length, dtype=jnp.int32)[None, :]
    weights = jnp.where(causal[:, :, None], jnp.exp(jnp.minimum(gap_matrix, 0.0)), 0.0)
    scores = jnp.einsum('ihd,jhd->ijh', queries, keys_rot, precision=highest) * weights
    inner_part = jnp.einsum('ijh,jhe->ihe', scores, values, precision=highest)
    cross_part = jnp.einsum('ihd,hde->ihe', queries, carry_state, precision=highest) * jnp.exp(cumulative)[:, :, None]
    total_log = cumulative[-1]
    tail_weight = jnp.exp(total_log[None, :] - cumulative)
    carried = carry_state * jnp.exp(total_log)[:, None, None] + jnp.einsum('jhd,jh,jhe->hde', keys_rot, tail_weight, values, precision=highest)
    return (carried, inner_part + cross_part)

def head_norm(retained, gain_row, gate_rows):
    mean_part = lax.optimization_barrier(jnp.mean(retained, axis=-1, keepdims=True))
    centred = retained - mean_part
    variance = lax.optimization_barrier(jnp.mean(centred * centred, axis=-1, keepdims=True))
    scaled = (centred * lax.rsqrt(variance + group_eps)).reshape(retained.shape[0], -1)
    return (scaled * gain_row * jax.nn.silu(gate_rows.astype(jnp.float32))).astype(jnp.bfloat16)

def square_norm(updated, gain_row):
    factor = lax.rsqrt(lax.optimization_barrier(jnp.mean(updated * updated, axis=-1, keepdims=True)) + square_eps)
    return (updated * factor * gain_row).astype(jnp.bfloat16)

def expert_rows(rows, gate_part, up_part):
    gate_pre = jnp.dot(rows, gate_part, preferred_element_type=jnp.float32)
    up_pre = jnp.dot(rows, up_part, preferred_element_type=jnp.float32)
    gate_clip = jnp.minimum(gate_pre, clamp_limit)
    up_clip = jnp.clip(up_pre, -clamp_limit, clamp_limit)
    return ((up_clip + 1.0) * (gate_clip * jax.nn.sigmoid(gate_clip * swish_alpha))).astype(jnp.bfloat16)

def slot_ranks(route_block, experts):
    flat_routes = route_block.reshape(-1)
    onehot = (flat_routes[:, None] == jnp.arange(experts, dtype=jnp.int32)[None, :]).astype(jnp.int32)
    return (flat_routes, lax.optimization_barrier(jnp.sum(jnp.cumsum(onehot, axis=0) * onehot, axis=1)) - 1)

def reference(query_rows, key_rows, value_rows, gate_rows, log_decay, head_gain, out_weight, residual, ffn_gain, gate_weight, up_weight, down_weight, routes, route_weights):
    positions = jnp.arange(TOKEN_TOTAL, dtype=jnp.float32)
    angles = rotary_angles(positions, HEAD_DIM)
    head_shape = (TOKEN_TOTAL, HEAD_TOTAL, HEAD_DIM)
    queries = rotate(query_rows.astype(jnp.float32).reshape(head_shape), angles)
    keys_rot = rotate(key_rows.astype(jnp.float32).reshape(head_shape), angles) * HEAD_DIM ** (-0.5)
    values = value_rows.astype(jnp.float32).reshape(head_shape)
    block_count = TOKEN_TOTAL // BLOCK

    def advance(carry_state, pieces):
        return block_pass(carry_state, pieces[0], pieces[1], pieces[2], pieces[3])
    start_state = jnp.zeros((HEAD_TOTAL, HEAD_DIM, HEAD_DIM), jnp.float32)
    block_shape = (block_count, BLOCK, HEAD_TOTAL, HEAD_DIM)
    _, retained = lax.scan(advance, start_state, (queries.reshape(block_shape), keys_rot.reshape(block_shape), values.reshape(block_shape), log_decay.reshape(block_count, BLOCK, HEAD_TOTAL)))
    retained = retained.reshape(head_shape)
    hidden = head_norm(retained, head_gain, gate_rows)
    updated = residual.astype(jnp.float32) + jnp.dot(hidden, out_weight, preferred_element_type=jnp.float32)
    ffn_in = square_norm(updated, ffn_gain)
    block_total = TOKEN_TOTAL // ROWS_DEV
    grouped = routes.reshape(block_total, ROWS_DEV, TOPK)
    flat_experts, flat_ranks = jax.vmap(partial(slot_ranks, experts=EXPERTS))(grouped)
    block_index = jnp.arange(block_total, dtype=jnp.int32)[:, None]
    slot_index = flat_experts * (block_total * CAP) + block_index * CAP + flat_ranks
    row_index = block_index * ROWS_DEV + jnp.arange(ROWS_DEV * TOPK, dtype=jnp.int32)[None, :] // TOPK
    source_row = jnp.full((EXPERTS * block_total * CAP,), TOKEN_TOTAL, jnp.int32).at[slot_index.reshape(-1)].set(row_index.reshape(-1))
    slot_weight = jnp.zeros((EXPERTS * block_total * CAP,), jnp.float32).at[slot_index.reshape(-1)].set(route_weights.reshape(-1))
    padded = jnp.concatenate([ffn_in, jnp.zeros((1, D), jnp.bfloat16)], axis=0)
    quarter = FF // N_TP

    def expert_step(accumulated, pieces):
        sources, weight_col, gate_part, up_part, down_part = pieces
        activity = expert_rows(padded[sources], gate_part, up_part)
        partials = jnp.einsum('mqf,qfd->qmd', activity.reshape(-1, N_TP, quarter).astype(jnp.float32), down_part.reshape(N_TP, quarter, D).astype(jnp.float32))
        rounded = lax.optimization_barrier(partials.astype(jnp.bfloat16)).astype(jnp.float32)
        expert_out = lax.optimization_barrier(jnp.sum(rounded, axis=0)).astype(jnp.bfloat16)
        return (accumulated.at[sources].add(weight_col[:, None] * expert_out.astype(jnp.float32)), None)
    start_sum = jnp.zeros((TOKEN_TOTAL + 1, D), jnp.float32)
    accumulated, _ = lax.scan(expert_step, start_sum, (source_row.reshape(EXPERTS, -1), slot_weight.reshape(EXPERTS, -1), gate_weight, up_weight, down_weight))
    return (updated + accumulated[:TOKEN_TOTAL]).astype(jnp.bfloat16)
```

```python
import functools

import jax
import jax.numpy as jnp
from jax import lax
from jax.experimental import pallas as pl
from jax.experimental.pallas import tpu as pltpu
from jax.sharding import PartitionSpec as P

HEAD_DIM = 128
TOPK = 4
BLOCK = 128


highest = lax.Precision.HIGHEST
rope_base = 10000.0
group_eps = 1e-05
square_eps = 1e-06
clamp_limit = 7.0
swish_alpha = 1.702


def rotary_angles(positions, head_dim):
    half_dim = head_dim // 2
    inverse = rope_base ** (-jnp.arange(half_dim, dtype=jnp.float32) / half_dim)
    return positions[:, None] * inverse[None, :]


def square_norm(updated, gain_row):
    factor = lax.rsqrt(jnp.mean(updated * updated, axis=-1, keepdims=True) + square_eps)
    return (updated * factor * gain_row).astype(jnp.bfloat16)


def expert_rows(rows, gate_part, up_part):
    gate_pre = jnp.dot(rows, gate_part, preferred_element_type=jnp.float32)
    up_pre = jnp.dot(rows, up_part, preferred_element_type=jnp.float32)
    gate_clip = jnp.minimum(gate_pre, clamp_limit)
    up_clip = jnp.clip(up_pre, -clamp_limit, clamp_limit)
    return ((up_clip + 1.0) * (gate_clip * jax.nn.sigmoid(gate_clip * swish_alpha))).astype(
        jnp.bfloat16
    )


def slot_ranks(route_block, experts):
    flat_routes = route_block.reshape(-1)
    onehot = (flat_routes[:, None] == jnp.arange(experts, dtype=jnp.int32)[None, :]).astype(
        jnp.int32
    )
    return (flat_routes, jnp.sum(jnp.cumsum(onehot, axis=0) * onehot, axis=1) - 1)


def retention_kernel(q_ref, k_ref, v_ref, cos_ref, sin_ref, cum_ref, cum_row_ref, ret_ref, qdec_ref, state_ref):
    head = pl.program_id(0)
    length = q_ref.shape[0]
    cosine, sine = cos_ref[...], sin_ref[...]
    half = HEAD_DIM // 2

    def turned(ref):
        rows = ref[...].astype(jnp.float32)
        return rows * cosine + pltpu.roll(rows, half, 1) * sine

    lanes = lax.broadcasted_iota(jnp.int32, cum_ref.shape, 1)
    column = jnp.sum(jnp.where(lanes == head, cum_ref[...], 0.0), axis=1, keepdims=True)
    row = cum_row_ref[0]
    queries = turned(q_ref)
    keys = turned(k_ref) * HEAD_DIM ** (-0.5)
    values = v_ref[...]
    scores = lax.dot_general(
        queries.astype(jnp.bfloat16),
        keys.astype(jnp.bfloat16),
        (((1,), (1,)), ((), ())),
        preferred_element_type=jnp.float32,
    )
    causal = lax.broadcasted_iota(jnp.int32, (length, length), 0) >= lax.broadcasted_iota(
        jnp.int32, (length, length), 1
    )
    weights = jnp.where(causal, jnp.exp(jnp.minimum(column - row, 0.0)), 0.0)
    ret_ref[...] = jnp.dot(
        (scores * weights).astype(jnp.bfloat16), values, preferred_element_type=jnp.float32
    )
    qdec_ref[...] = (queries * jnp.exp(column)).astype(jnp.bfloat16)
    total = column[length - 1 :, :]
    tailed = (keys * jnp.exp(total - column)).astype(jnp.bfloat16)
    state_ref[0, :HEAD_DIM, :] = lax.dot_general(
        tailed, values, (((0,), (0,)), ((), ())), preferred_element_type=jnp.float32
    )
    state_ref[0, HEAD_DIM:, :] = jnp.broadcast_to(total, (8, HEAD_DIM))


def norm_kernel(ret_ref, qdec_ref, enter_ref, gain_ref, gate_ref, hidden_ref):
    retained = ret_ref[...] + jnp.dot(
        qdec_ref[...], enter_ref[0].astype(jnp.bfloat16), preferred_element_type=jnp.float32
    )
    centred = retained - jnp.mean(retained, axis=-1, keepdims=True)
    variance = jnp.mean(centred * centred, axis=-1, keepdims=True)
    gate = gate_ref[...].astype(jnp.float32)
    scaled = centred * lax.rsqrt(variance + group_eps) * gain_ref[...]
    hidden_ref[...] = (scaled * (gate / (1.0 + jnp.exp(-gate)))).astype(jnp.bfloat16)


def retention(query_rows, key_rows, value_rows, gate_rows, log_decay, head_gain):
    length, local_heads = log_decay.shape
    width = query_rows.shape[1]
    sp_count, mine = lax.axis_size("sp"), lax.axis_index("sp")
    positions = (mine * length + jnp.arange(length, dtype=jnp.int32)).astype(jnp.float32)
    angles = rotary_angles(positions, HEAD_DIM)
    cosine, sine = jnp.cos(angles), jnp.sin(angles)
    cosine = jnp.concatenate([cosine, cosine], axis=1)
    sine = jnp.concatenate([-sine, sine], axis=1)
    cumulative = jnp.cumsum(log_decay, axis=0)
    rows_spec = pl.BlockSpec((length, HEAD_DIM), lambda h: (0, h))
    table_spec = pl.BlockSpec((length, HEAD_DIM), lambda h: (0, 0))
    retained, qdec, state = pl.pallas_call(
        retention_kernel,
        grid=(local_heads,),
        out_shape=(
            jax.ShapeDtypeStruct((length, width), jnp.float32),
            jax.ShapeDtypeStruct((length, width), jnp.bfloat16),
            jax.ShapeDtypeStruct((local_heads, HEAD_DIM + 8, HEAD_DIM), jnp.float32),
        ),
        in_specs=[
            rows_spec,
            rows_spec,
            rows_spec,
            table_spec,
            table_spec,
            pl.BlockSpec((length, local_heads), lambda h: (0, 0)),
            pl.BlockSpec((1, 1, length), lambda h: (h, 0, 0)),
        ],
        out_specs=(
            rows_spec,
            rows_spec,
            pl.BlockSpec((1, HEAD_DIM + 8, HEAD_DIM), lambda h: (h, 0, 0)),
        ),
    )(query_rows, key_rows, value_rows, cosine, sine, cumulative, cumulative.T[:, None, :])
    pieces = lax.all_gather(state, "sp")
    totals = pieces[:, :, HEAD_DIM, 0]
    index = jnp.arange(sp_count, dtype=jnp.int32)
    between = (index[None, :] > index[:, None]) & (index[None, :] < mine)
    gap = jnp.sum(jnp.where(between[:, :, None], totals[None], 0.0), axis=1)
    factor = jnp.where((index < mine)[:, None], jnp.exp(gap), 0.0)
    entering = jnp.sum(factor[:, :, None, None] * pieces[:, :, :HEAD_DIM, :], axis=0)
    return pl.pallas_call(
        norm_kernel,
        grid=(local_heads,),
        out_shape=jax.ShapeDtypeStruct((length, width), jnp.bfloat16),
        in_specs=[
            rows_spec,
            rows_spec,
            pl.BlockSpec((1, HEAD_DIM, HEAD_DIM), lambda h: (h, 0, 0)),
            pl.BlockSpec((1, HEAD_DIM), lambda h: (0, h)),
            rows_spec,
        ],
        out_specs=rows_spec,
    )(retained, qdec, entering, head_gain[None, :], gate_rows)


def dense_experts(updated, ffn_in, own_routes, route_weights, gate_part, up_part, down_part):
    sp_count, mine = lax.axis_size("sp"), lax.axis_index("sp")
    width = ffn_in.shape[1]
    chosen = own_routes[:, :, None] == jnp.arange(sp_count, dtype=jnp.int32)[None, None, :]
    shares = jnp.sum(jnp.where(chosen, route_weights[:, :, None], 0.0), axis=1)
    coarse = shares.astype(jnp.bfloat16)
    fine = (shares - coarse.astype(jnp.float32)).astype(jnp.bfloat16)
    spare = jnp.zeros((ffn_in.shape[0], 128 - 2 * sp_count), jnp.bfloat16)
    payload = jnp.concatenate([ffn_in, coarse, fine, spare], axis=1)
    everyone = lax.all_gather(payload, ("sp", "tp"), axis=0, tiled=True)
    rows = everyone[:, :width]
    tail = everyone[:, width:].astype(jnp.float32)
    lane = jnp.arange(128, dtype=jnp.int32)[None, :]
    weight = jnp.sum(
        jnp.where((lane == mine) | (lane == mine + sp_count), tail, 0.0), axis=1, keepdims=True
    )
    activity = expert_rows(rows, gate_part, up_part)
    partial_out = jnp.dot(activity, down_part, preferred_element_type=jnp.float32) * weight
    summed = lax.psum_scatter(
        partial_out.astype(jnp.bfloat16), ("sp", "tp"), scatter_dimension=0, tiled=True
    )
    return (updated + summed.astype(jnp.float32)).astype(jnp.bfloat16)


def body(
    query_rows,
    key_rows,
    value_rows,
    gate_rows,
    log_decay,
    head_gain,
    out_weight,
    residual,
    ffn_gain,
    gate_weight,
    up_weight,
    down_weight,
    routes,
    route_weights,
):
    tok_count = query_rows.shape[0]
    local_heads = log_decay.shape[1]
    sp_count = lax.axis_size("sp")
    tp_count = lax.axis_size("tp")
    model_width = residual.shape[1]
    rows_own = tok_count // tp_count
    capacity = max(2, 3 * rows_own * TOPK // (2 * sp_count))
    hidden = retention(query_rows, key_rows, value_rows, gate_rows, log_decay, head_gain)
    mixed_sum = lax.psum_scatter(
        jnp.dot(hidden, out_weight, preferred_element_type=jnp.float32).astype(jnp.bfloat16),
        "tp",
        scatter_dimension=0,
        tiled=True,
    ).astype(jnp.float32)
    updated = residual.astype(jnp.float32) + mixed_sum
    ffn_in = square_norm(updated, ffn_gain)
    tp_index = lax.axis_index("tp")
    own_routes = lax.dynamic_slice_in_dim(routes, tp_index * rows_own, rows_own, 0)
    if rows_own < 2 * capacity and 2 * sp_count <= 128:
        return dense_experts(
            updated, ffn_in, own_routes, route_weights, gate_weight[0], up_weight[0], down_weight[0]
        )
    own_experts, own_ranks = slot_ranks(own_routes, sp_count)
    home_slot = own_experts * capacity + own_ranks
    gate_part = gate_weight[0]
    up_part = up_weight[0]
    down_part = down_weight[0]
    empty_row = jnp.zeros((1, model_width), jnp.bfloat16)
    source_row = (
        jnp.full((sp_count * capacity,), rows_own, jnp.int32)
        .at[home_slot]
        .set(jnp.arange(rows_own * TOPK, dtype=jnp.int32) // TOPK)
    )
    padded = jnp.concatenate([ffn_in, empty_row], axis=0)
    outgoing = padded[source_row].reshape(sp_count, capacity, model_width)
    arrived = lax.all_to_all(outgoing, "sp", split_axis=0, concat_axis=0, tiled=True)
    fanned = lax.all_gather(arrived[None], "tp", axis=0, tiled=True)
    activity = expert_rows(fanned.reshape(-1, model_width), gate_part, up_part)
    partial_out = jnp.dot(activity, down_part, preferred_element_type=jnp.float32).reshape(
        tp_count, sp_count, capacity, model_width
    )
    summed = (
        lax.psum_scatter(partial_out.astype(jnp.bfloat16), "tp", scatter_dimension=0, tiled=True)
        .astype(jnp.float32)
        .reshape(sp_count, capacity, model_width)
    )
    returned = lax.all_to_all(
        summed.astype(jnp.bfloat16), "sp", split_axis=0, concat_axis=0, tiled=True
    )
    picked = returned.reshape(sp_count * capacity, model_width)[home_slot].reshape(
        rows_own, TOPK, model_width
    )
    expert_sum = jnp.sum(route_weights[:, :, None] * picked.astype(jnp.float32), axis=1)
    return (updated + expert_sum).astype(jnp.bfloat16)


def solution(mesh):
    return jax.shard_map(
        body,
        mesh=mesh,
        in_specs=(
            P("sp", "tp"),
            P("sp", "tp"),
            P("sp", "tp"),
            P("sp", "tp"),
            P("sp", "tp"),
            P("tp"),
            P("tp", None),
            P(("sp", "tp"), None),
            P(),
            P("sp", None, "tp"),
            P("sp", None, "tp"),
            P("sp", "tp", None),
            P("sp", None),
            P(("sp", "tp"), None),
        ),
        out_specs=P(("sp", "tp"), None),
        check_vma=False,
    )
```

```python
import functools

import jax
import jax.numpy as jnp
from jax import lax
from jax.experimental import pallas as pl
from jax.experimental.pallas import tpu as pltpu
from jax.sharding import PartitionSpec as P

HEAD_DIM = 128
TOPK = 4
BLOCK = 128


highest = lax.Precision.HIGHEST
rope_base = 10000.0
group_eps = 1e-05
square_eps = 1e-06
clamp_limit = 7.0
swish_alpha = 1.702


def rotary_angles(positions, head_dim):
    half_dim = head_dim // 2
    inverse = rope_base ** (-jnp.arange(half_dim, dtype=jnp.float32) / half_dim)
    return positions[:, None] * inverse[None, :]


def square_norm(updated, gain_row):
    factor = lax.rsqrt(jnp.mean(updated * updated, axis=-1, keepdims=True) + square_eps)
    return (updated * factor * gain_row).astype(jnp.bfloat16)


def expert_rows(rows, gate_part, up_part):
    gate_pre = jnp.dot(rows, gate_part, preferred_element_type=jnp.float32)
    up_pre = jnp.dot(rows, up_part, preferred_element_type=jnp.float32)
    gate_clip = jnp.minimum(gate_pre, clamp_limit)
    up_clip = jnp.clip(up_pre, -clamp_limit, clamp_limit)
    return ((up_clip + 1.0) * (gate_clip * jax.nn.sigmoid(gate_clip * swish_alpha))).astype(
        jnp.bfloat16
    )


def slot_ranks(route_block, experts):
    flat_routes = route_block.reshape(-1)
    onehot = (flat_routes[:, None] == jnp.arange(experts, dtype=jnp.int32)[None, :]).astype(
        jnp.int32
    )
    return (flat_routes, jnp.sum(jnp.cumsum(onehot, axis=0) * onehot, axis=1) - 1)


def retention_kernel(q_ref, k_ref, v_ref, cos_ref, sin_ref, cum_ref, cum_row_ref, ret_ref, qdec_ref, state_ref):
    head = pl.program_id(0)
    length = q_ref.shape[0]
    cosine, sine = cos_ref[...], sin_ref[...]
    half = HEAD_DIM // 2

    def turned(ref):
        rows = ref[...].astype(jnp.float32)
        return rows * cosine + pltpu.roll(rows, half, 1) * sine

    lanes = lax.broadcasted_iota(jnp.int32, cum_ref.shape, 1)
    column = jnp.sum(jnp.where(lanes == head, cum_ref[...], 0.0), axis=1, keepdims=True)
    row = cum_row_ref[0]
    queries = turned(q_ref)
    keys = turned(k_ref) * HEAD_DIM ** (-0.5)
    values = v_ref[...]
    scores = lax.dot_general(
        queries.astype(jnp.bfloat16),
        keys.astype(jnp.bfloat16),
        (((1,), (1,)), ((), ())),
        preferred_element_type=jnp.float32,
    )
    causal = lax.broadcasted_iota(jnp.int32, (length, length), 0) >= lax.broadcasted_iota(
        jnp.int32, (length, length), 1
    )
    weights = jnp.where(causal, jnp.exp(jnp.minimum(column - row, 0.0)), 0.0)
    ret_ref[...] = jnp.dot(
        (scores * weights).astype(jnp.bfloat16), values, preferred_element_type=jnp.float32
    )
    qdec_ref[...] = (queries * jnp.exp(column)).astype(jnp.bfloat16)
    total = column[length - 1 :, :]
    tailed = (keys * jnp.exp(total - column)).astype(jnp.bfloat16)
    state_ref[0, :HEAD_DIM, :] = lax.dot_general(
        tailed, values, (((0,), (0,)), ((), ())), preferred_element_type=jnp.float32
    )
    state_ref[0, HEAD_DIM:, :] = jnp.broadcast_to(total, (8, HEAD_DIM))


def norm_kernel(ret_ref, qdec_ref, enter_ref, gain_ref, gate_ref, hidden_ref):
    retained = ret_ref[...] + jnp.dot(
        qdec_ref[...], enter_ref[0].astype(jnp.bfloat16), preferred_element_type=jnp.float32
    )
    centred = retained - jnp.mean(retained, axis=-1, keepdims=True)
    variance = jnp.mean(centred * centred, axis=-1, keepdims=True)
    gate = gate_ref[...].astype(jnp.float32)
    scaled = centred * lax.rsqrt(variance + group_eps) * gain_ref[...]
    hidden_ref[...] = (scaled * (gate / (1.0 + jnp.exp(-gate)))).astype(jnp.bfloat16)


def retention(query_rows, key_rows, value_rows, gate_rows, log_decay, head_gain):
    length, local_heads = log_decay.shape
    width = query_rows.shape[1]
    sp_count, mine = lax.axis_size("sp"), lax.axis_index("sp")
    positions = (mine * length + jnp.arange(length, dtype=jnp.int32)).astype(jnp.float32)
    angles = rotary_angles(positions, HEAD_DIM)
    cosine, sine = jnp.cos(angles), jnp.sin(angles)
    cosine = jnp.concatenate([cosine, cosine], axis=1)
    sine = jnp.concatenate([-sine, sine], axis=1)
    cumulative = jnp.cumsum(log_decay, axis=0)
    rows_spec = pl.BlockSpec((length, HEAD_DIM), lambda h: (0, h))
    table_spec = pl.BlockSpec((length, HEAD_DIM), lambda h: (0, 0))
    retained, qdec, state = pl.pallas_call(
        retention_kernel,
        grid=(local_heads,),
        out_shape=(
            jax.ShapeDtypeStruct((length, width), jnp.float32),
            jax.ShapeDtypeStruct((length, width), jnp.bfloat16),
            jax.ShapeDtypeStruct((local_heads, HEAD_DIM + 8, HEAD_DIM), jnp.float32),
        ),
        in_specs=[
            rows_spec,
            rows_spec,
            rows_spec,
            table_spec,
            table_spec,
            pl.BlockSpec((length, local_heads), lambda h: (0, 0)),
            pl.BlockSpec((1, 1, length), lambda h: (h, 0, 0)),
        ],
        out_specs=(
            rows_spec,
            rows_spec,
            pl.BlockSpec((1, HEAD_DIM + 8, HEAD_DIM), lambda h: (h, 0, 0)),
        ),
    )(query_rows, key_rows, value_rows, cosine, sine, cumulative, cumulative.T[:, None, :])
    pieces = lax.all_gather(state, "sp")
    totals = pieces[:, :, HEAD_DIM, 0]
    index = jnp.arange(sp_count, dtype=jnp.int32)
    between = (index[None, :] > index[:, None]) & (index[None, :] < mine)
    gap = jnp.sum(jnp.where(between[:, :, None], totals[None], 0.0), axis=1)
    factor = jnp.where((index < mine)[:, None], jnp.exp(gap), 0.0)
    entering = jnp.sum(factor[:, :, None, None] * pieces[:, :, :HEAD_DIM, :], axis=0)
    return pl.pallas_call(
        norm_kernel,
        grid=(local_heads,),
        out_shape=jax.ShapeDtypeStruct((length, width), jnp.bfloat16),
        in_specs=[
            rows_spec,
            rows_spec,
            pl.BlockSpec((1, HEAD_DIM, HEAD_DIM), lambda h: (h, 0, 0)),
            pl.BlockSpec((1, HEAD_DIM), lambda h: (0, h)),
            rows_spec,
        ],
        out_specs=rows_spec,
    )(retained, qdec, entering, head_gain[None, :], gate_rows)


Z_A, Z_B, X_A2, Y_B2, Y_A3, Y_A4, X_B3, X_B4, C_A, C_B, C_P, Y_A, X_B, X_A, Y_B, RZ_A, RZ_B = range(17)


def experts_kernel(
    planes, x0, x1, upd, wg, wu, wd, out,
    g0, g1, pm, pc, pr, a0, a1, r10, r11, b0, b1, r20, r21, d0, d1, z0, z1,
    ssem, rsem, lsem,
):
    sp, tp = lax.axis_index("sp"), lax.axis_index("tp")
    sp_count = 2 * planes
    z, x = sp // 2, sp % 2
    y, c = tp // 2, tp % 2
    half = x1.shape[1]
    rows = x1.shape[0]
    f32, bf16 = jnp.float32, jnp.bfloat16
    to_core = {"sp": sp, "tp": y * 2 + (1 - c)}
    to_y = {"sp": sp, "tp": (1 - y) * 2 + c}
    to_x = {"sp": z * 2 + (1 - x), "tp": tp}

    def plane_of(i):
        return (z + planes - i) % planes

    def to_z(i):
        return {"sp": plane_of(i) * 2 + x, "tp": tp}

    def from_z(i):
        return {"sp": ((z + i) % planes) * 2 + x, "tp": tp}

    def move(kind, i, src, dst, device):
        return pltpu.make_async_remote_copy(
            src_ref=src, dst_ref=dst, send_sem=ssem.at[kind, i], recv_sem=rsem.at[kind, i],
            device_id=device, device_id_type=pl.DeviceIdType.MESH,
        )

    def send(kind, i, src, dst, device):
        move(kind, i, src, dst, device).start()

    def arrived(kind, i, dst):
        move(kind, i, dst, dst, to_core).wait_recv()

    def left(kind, i, src):
        move(kind, i, src, src, to_core).wait_send()

    barrier = pltpu.get_barrier_semaphore()
    for device in [to_core, to_y, to_x] + [to_z(i) for i in range(1, planes)]:
        pl.semaphore_signal(barrier, inc=1, device_id=device, device_id_type=pl.DeviceIdType.MESH)
    pl.semaphore_wait(barrier, 2 + planes)

    here = x * 2 + y
    other_x = (1 - x) * 2 + y
    other_y = x * 2 + (1 - y)
    other_xy = (1 - x) * 2 + (1 - y)
    own0 = pltpu.make_async_copy(x0, g0.at[c, z, here], lsem.at[0])
    own1 = pltpu.make_async_copy(x1, g1.at[c, z, here], lsem.at[1])
    own0.start()
    own1.start()
    own0.wait()
    own1.wait()
    for i in range(1, planes):
        send(Z_A, i, g0.at[c, z, here], g0.at[c, z, here], from_z(i))
        send(Z_B, i, g1.at[c, z, here], g1.at[c, z, here], from_z(i))

    def compute(i, core):
        p = plane_of(i)
        left_rows = g0[core, p].reshape(4 * rows, half + 128)
        right_rows = g1[core, p].reshape(4 * rows, half)
        tail = left_rows[:, half:].astype(f32)
        left_rows = left_rows[:, :half]
        lane = lax.broadcasted_iota(jnp.int32, tail.shape, 1)
        weight = jnp.sum(
            jnp.where((lane == sp) | (lane == sp + sp_count), tail, 0.0), axis=1, keepdims=True
        )

        def product(w):
            return jnp.dot(left_rows, w[:half, :], preferred_element_type=f32) + jnp.dot(
                right_rows, w[half:, :], preferred_element_type=f32
            )

        gate = jnp.minimum(product(wg), clamp_limit)
        up = jnp.clip(product(wu), -clamp_limit, clamp_limit)
        act = ((up + 1.0) * (gate / (1.0 + jnp.exp(-swish_alpha * gate)))).astype(bf16)
        return (jnp.dot(act, wd[...], preferred_element_type=f32) * weight).astype(bf16)

    def step(i, carry):
        @pl.when((i >= 1) & (i < planes + 1))
        def _():
            j = i - 1
            p = plane_of(j)
            arrived(Y_A3, j, g0.at[c, p, other_y])
            arrived(Y_A4, j, g0.at[c, p, other_xy])
            arrived(X_B3, j, g1.at[c, p, other_x])
            arrived(X_B4, j, g1.at[c, p, other_xy])
            send(C_A, j, g0.at[c, p], g0.at[c, p], to_core)
            send(C_B, j, g1.at[c, p], g1.at[c, p], to_core)

        @pl.when(i < planes)
        def _():
            p = plane_of(i)

            @pl.when(i > 0)
            def _():
                arrived(Z_A, i, g0.at[c, p, here])
                arrived(Z_B, i, g1.at[c, p, here])

            send(X_A2, i, g0.at[c, p, here], g0.at[c, p, here], to_x)
            send(Y_B2, i, g1.at[c, p, here], g1.at[c, p, here], to_y)
            send(Y_A3, i, g0.at[c, p, here], g0.at[c, p, here], to_y)
            send(X_B3, i, g1.at[c, p, here], g1.at[c, p, here], to_x)
            arrived(X_A2, i, g0.at[c, p, other_x])
            send(Y_A4, i, g0.at[c, p, other_x], g0.at[c, p, other_x], to_y)
            arrived(Y_B2, i, g1.at[c, p, other_y])
            send(X_B4, i, g1.at[c, p, other_y], g1.at[c, p, other_y], to_x)

        @pl.when((i >= 2) & (i < planes + 2))
        def _():
            j = i - 2
            arrived(C_P, j, pr.at[j])
            for q in range(4):
                part = pl.ds(q * rows, rows)
                total = (pm[j, part, :].astype(f32) + pr[j, part, :].astype(f32)).astype(bf16)
                a0[j, q % 2, q // 2] = total[:, :half]
                a1[j, q // 2, q % 2] = total[:, half:]
            send(Y_A, j, a0.at[j, 1 - y], r10.at[j], to_y)
            send(X_B, j, a1.at[j, 1 - x], r11.at[j], to_x)

        @pl.when((i >= 3) & (i < planes + 3))
        def _():
            j = i - 3
            arrived(Y_A, j, r10.at[j])
            b0[j] = (a0[j, y].astype(f32) + r10[j].astype(f32)).astype(bf16)
            send(X_A, j, b0.at[j, 1 - x], r20.at[j], to_x)
            arrived(X_B, j, r11.at[j])
            b1[j] = (a1[j, x].astype(f32) + r11[j].astype(f32)).astype(bf16)
            send(Y_B, j, b1.at[j, 1 - y], r21.at[j], to_y)

        @pl.when((i >= 4) & (i < planes + 4))
        def _():
            j = i - 4
            arrived(X_A, j, r20.at[j])
            d0[j] = (b0[j, x].astype(f32) + r20[j].astype(f32)).astype(bf16)
            arrived(Y_B, j, r21.at[j])
            d1[j] = (b1[j, y].astype(f32) + r21[j].astype(f32)).astype(bf16)

            @pl.when(j > 0)
            def _():
                send(RZ_A, j, d0.at[j], z0.at[j], to_z(j))
                send(RZ_B, j, d1.at[j], z1.at[j], to_z(j))

        @pl.when((i >= 1) & (i < planes + 1))
        def _():
            j = i - 1
            p = plane_of(j)
            arrived(C_A, j, g0.at[1 - c, p])
            arrived(C_B, j, g1.at[1 - c, p])

            def tile(turn, carry):
                @pl.when(turn == 0)
                def _():
                    pc[j] = compute(j, 1 - c)
                    send(C_P, j, pc.at[j], pr.at[j], to_core)

                @pl.when(turn == 1)
                def _():
                    pm[j] = compute(j, c)

                return carry

            lax.fori_loop(0, 2, tile, 0)

        return carry

    lax.fori_loop(0, planes + 4, step, 0)
    low, high = upd[:, :half], upd[:, half:]
    low = low + d0[0].astype(f32)
    high = high + d1[0].astype(f32)
    for i in range(1, planes):
        arrived(RZ_A, i, z0.at[i])
        low = low + z0[i].astype(f32)
        arrived(RZ_B, i, z1.at[i])
        high = high + z1[i].astype(f32)
    out[:, :half] = low.astype(bf16)
    out[:, half:] = high.astype(bf16)

    def drain(i, carry):
        p = plane_of(i)

        @pl.when(i > 0)
        def _():
            left(Z_A, i, g0.at[c, z, here])
            left(Z_B, i, g1.at[c, z, here])
            left(RZ_A, i, d0.at[i])
            left(RZ_B, i, d1.at[i])

        left(X_A2, i, g0.at[c, p, here])
        left(Y_B2, i, g1.at[c, p, here])
        left(Y_A3, i, g0.at[c, p, here])
        left(X_B3, i, g1.at[c, p, here])
        left(Y_A4, i, g0.at[c, p, other_x])
        left(X_B4, i, g1.at[c, p, other_y])
        left(C_A, i, g0.at[c, p])
        left(C_B, i, g1.at[c, p])
        left(C_P, i, pc.at[i])
        left(Y_A, i, a0.at[i, 1 - y])
        left(X_B, i, a1.at[i, 1 - x])
        left(X_A, i, b0.at[i, 1 - x])
        left(Y_B, i, b1.at[i, 1 - y])
        return carry

    lax.fori_loop(0, planes, drain, 0)


def dense_experts(updated, ffn_in, own_routes, route_weights, gate_part, up_part, down_part):
    sp_count, mine = lax.axis_size("sp"), lax.axis_index("sp")
    width = ffn_in.shape[1]
    chosen = own_routes[:, :, None] == jnp.arange(sp_count, dtype=jnp.int32)[None, None, :]
    shares = jnp.sum(jnp.where(chosen, route_weights[:, :, None], 0.0), axis=1)
    coarse = shares.astype(jnp.bfloat16)
    fine = (shares - coarse.astype(jnp.float32)).astype(jnp.bfloat16)
    spare = jnp.zeros((ffn_in.shape[0], 128 - 2 * sp_count), jnp.bfloat16)
    half = width // 2
    first = jnp.concatenate([ffn_in[:, :half], coarse, fine, spare], axis=1)
    second = ffn_in[:, half:]
    rows = ffn_in.shape[0]
    planes = sp_count // 2
    bf16 = jnp.bfloat16
    whole = pl.BlockSpec(memory_space=pltpu.VMEM)
    return pl.pallas_call(
        functools.partial(experts_kernel, planes),
        out_shape=jax.ShapeDtypeStruct((rows, width), bf16),
        in_specs=[whole] * 6,
        out_specs=whole,
        scratch_shapes=[
            pltpu.VMEM((2, planes, 4, rows, half + 128), bf16),
            pltpu.VMEM((2, planes, 4, rows, half), bf16),
            pltpu.VMEM((planes, 4 * rows, width), bf16),
            pltpu.VMEM((planes, 4 * rows, width), bf16),
            pltpu.VMEM((planes, 4 * rows, width), bf16),
            pltpu.VMEM((planes, 2, 2, rows, half), bf16),
            pltpu.VMEM((planes, 2, 2, rows, half), bf16),
            pltpu.VMEM((planes, 2, rows, half), bf16),
            pltpu.VMEM((planes, 2, rows, half), bf16),
            pltpu.VMEM((planes, 2, rows, half), bf16),
            pltpu.VMEM((planes, 2, rows, half), bf16),
            pltpu.VMEM((planes, rows, half), bf16),
            pltpu.VMEM((planes, rows, half), bf16),
            pltpu.VMEM((planes, rows, half), bf16),
            pltpu.VMEM((planes, rows, half), bf16),
            pltpu.VMEM((planes, rows, half), bf16),
            pltpu.VMEM((planes, rows, half), bf16),
            pltpu.SemaphoreType.DMA((17, planes)),
            pltpu.SemaphoreType.DMA((17, planes)),
            pltpu.SemaphoreType.DMA((2,)),
        ],
        compiler_params=pltpu.CompilerParams(
            collective_id=0, has_side_effects=True, vmem_limit_bytes=63 * 1024 * 1024
        ),
    )(first, second, updated, gate_part, up_part, down_part)


def body(
    query_rows,
    key_rows,
    value_rows,
    gate_rows,
    log_decay,
    head_gain,
    out_weight,
    residual,
    ffn_gain,
    gate_weight,
    up_weight,
    down_weight,
    routes,
    route_weights,
):
    tok_count = query_rows.shape[0]
    local_heads = log_decay.shape[1]
    sp_count = lax.axis_size("sp")
    tp_count = lax.axis_size("tp")
    model_width = residual.shape[1]
    rows_own = tok_count // tp_count
    capacity = max(2, 3 * rows_own * TOPK // (2 * sp_count))
    hidden = retention(query_rows, key_rows, value_rows, gate_rows, log_decay, head_gain)
    mixed_sum = lax.psum_scatter(
        jnp.dot(hidden, out_weight, preferred_element_type=jnp.float32).astype(jnp.bfloat16),
        "tp",
        scatter_dimension=0,
        tiled=True,
    ).astype(jnp.float32)
    updated = residual.astype(jnp.float32) + mixed_sum
    ffn_in = square_norm(updated, ffn_gain)
    tp_index = lax.axis_index("tp")
    own_routes = lax.dynamic_slice_in_dim(routes, tp_index * rows_own, rows_own, 0)
    if rows_own < 2 * capacity and 2 * sp_count <= 128 and sp_count % 2 == 0 and tp_count == 4:
        return dense_experts(
            updated, ffn_in, own_routes, route_weights, gate_weight[0], up_weight[0], down_weight[0]
        )
    own_experts, own_ranks = slot_ranks(own_routes, sp_count)
    home_slot = own_experts * capacity + own_ranks
    gate_part = gate_weight[0]
    up_part = up_weight[0]
    down_part = down_weight[0]
    empty_row = jnp.zeros((1, model_width), jnp.bfloat16)
    source_row = (
        jnp.full((sp_count * capacity,), rows_own, jnp.int32)
        .at[home_slot]
        .set(jnp.arange(rows_own * TOPK, dtype=jnp.int32) // TOPK)
    )
    padded = jnp.concatenate([ffn_in, empty_row], axis=0)
    outgoing = padded[source_row].reshape(sp_count, capacity, model_width)
    arrived = lax.all_to_all(outgoing, "sp", split_axis=0, concat_axis=0, tiled=True)
    fanned = lax.all_gather(arrived[None], "tp", axis=0, tiled=True)
    activity = expert_rows(fanned.reshape(-1, model_width), gate_part, up_part)
    partial_out = jnp.dot(activity, down_part, preferred_element_type=jnp.float32).reshape(
        tp_count, sp_count, capacity, model_width
    )
    summed = (
        lax.psum_scatter(partial_out.astype(jnp.bfloat16), "tp", scatter_dimension=0, tiled=True)
        .astype(jnp.float32)
        .reshape(sp_count, capacity, model_width)
    )
    returned = lax.all_to_all(
        summed.astype(jnp.bfloat16), "sp", split_axis=0, concat_axis=0, tiled=True
    )
    picked = returned.reshape(sp_count * capacity, model_width)[home_slot].reshape(
        rows_own, TOPK, model_width
    )
    expert_sum = jnp.sum(route_weights[:, :, None] * picked.astype(jnp.float32), axis=1)
    return (updated + expert_sum).astype(jnp.bfloat16)


def solution(mesh):
    return jax.shard_map(
        body,
        mesh=mesh,
        in_specs=(
            P("sp", "tp"),
            P("sp", "tp"),
            P("sp", "tp"),
            P("sp", "tp"),
            P("sp", "tp"),
            P("tp"),
            P("tp", None),
            P(("sp", "tp"), None),
            P(),
            P("sp", None, "tp"),
            P("sp", None, "tp"),
            P("sp", "tp", None),
            P("sp", None),
            P(("sp", "tp"), None),
        ),
        out_specs=P(("sp", "tp"), None),
        check_vma=False,
    )
```

```python
import functools

import jax
import jax.numpy as jnp
from jax import lax
from jax.experimental import pallas as pl
from jax.experimental.pallas import tpu as pltpu
from jax.sharding import PartitionSpec as P

HEAD_DIM = 128
TOPK = 4
BLOCK = 128


highest = lax.Precision.HIGHEST
rope_base = 10000.0
group_eps = 1e-05
square_eps = 1e-06
clamp_limit = 7.0
swish_alpha = 1.702


def rotary_angles(positions, head_dim):
    half_dim = head_dim // 2
    inverse = rope_base ** (-jnp.arange(half_dim, dtype=jnp.float32) / half_dim)
    return positions[:, None] * inverse[None, :]


def square_norm(updated, gain_row):
    factor = lax.rsqrt(jnp.mean(updated * updated, axis=-1, keepdims=True) + square_eps)
    return (updated * factor * gain_row).astype(jnp.bfloat16)


def expert_rows(rows, gate_part, up_part):
    gate_pre = jnp.dot(rows, gate_part, preferred_element_type=jnp.float32)
    up_pre = jnp.dot(rows, up_part, preferred_element_type=jnp.float32)
    gate_clip = jnp.minimum(gate_pre, clamp_limit)
    up_clip = jnp.clip(up_pre, -clamp_limit, clamp_limit)
    return ((up_clip + 1.0) * (gate_clip * jax.nn.sigmoid(gate_clip * swish_alpha))).astype(
        jnp.bfloat16
    )


def slot_ranks(route_block, experts):
    flat_routes = route_block.reshape(-1)
    onehot = (flat_routes[:, None] == jnp.arange(experts, dtype=jnp.int32)[None, :]).astype(
        jnp.int32
    )
    return (flat_routes, jnp.sum(jnp.cumsum(onehot, axis=0) * onehot, axis=1) - 1)


def retention_kernel(q_ref, k_ref, v_ref, cos_ref, sin_ref, cum_ref, cum_row_ref, ret_ref, qdec_ref, state_ref):
    head = pl.program_id(0)
    length = q_ref.shape[0]
    cosine, sine = cos_ref[...], sin_ref[...]
    half = HEAD_DIM // 2

    def turned(ref):
        rows = ref[...].astype(jnp.float32)
        return rows * cosine + pltpu.roll(rows, half, 1) * sine

    lanes = lax.broadcasted_iota(jnp.int32, cum_ref.shape, 1)
    column = jnp.sum(jnp.where(lanes == head, cum_ref[...], 0.0), axis=1, keepdims=True)
    row = cum_row_ref[0]
    queries = turned(q_ref)
    keys = turned(k_ref) * HEAD_DIM ** (-0.5)
    values = v_ref[...]
    scores = lax.dot_general(
        queries.astype(jnp.bfloat16),
        keys.astype(jnp.bfloat16),
        (((1,), (1,)), ((), ())),
        preferred_element_type=jnp.float32,
    )
    causal = lax.broadcasted_iota(jnp.int32, (length, length), 0) >= lax.broadcasted_iota(
        jnp.int32, (length, length), 1
    )
    weights = jnp.where(causal, jnp.exp(jnp.minimum(column - row, 0.0)), 0.0)
    ret_ref[...] = jnp.dot(
        (scores * weights).astype(jnp.bfloat16), values, preferred_element_type=jnp.float32
    )
    qdec_ref[...] = (queries * jnp.exp(column)).astype(jnp.bfloat16)
    total = column[length - 1 :, :]
    tailed = (keys * jnp.exp(total - column)).astype(jnp.bfloat16)
    state_ref[0, :HEAD_DIM, :] = lax.dot_general(
        tailed, values, (((0,), (0,)), ((), ())), preferred_element_type=jnp.float32
    )
    state_ref[0, HEAD_DIM:, :] = jnp.broadcast_to(total, (8, HEAD_DIM))


def norm_kernel(ret_ref, qdec_ref, enter_ref, gain_ref, gate_ref, hidden_ref):
    retained = ret_ref[...] + jnp.dot(
        qdec_ref[...], enter_ref[0].astype(jnp.bfloat16), preferred_element_type=jnp.float32
    )
    centred = retained - jnp.mean(retained, axis=-1, keepdims=True)
    variance = jnp.mean(centred * centred, axis=-1, keepdims=True)
    gate = gate_ref[...].astype(jnp.float32)
    scaled = centred * lax.rsqrt(variance + group_eps) * gain_ref[...]
    hidden_ref[...] = (scaled * (gate / (1.0 + jnp.exp(-gate)))).astype(jnp.bfloat16)


def greet(devices):
    barrier = pltpu.get_barrier_semaphore()
    for device in devices:
        pl.semaphore_signal(barrier, inc=1, device_id=device, device_id_type=pl.DeviceIdType.MESH)
    pl.semaphore_wait(barrier, len(devices))


def state_kernel(planes, state, totals, entering, gs, gt, ssem, rsem, lsem):
    sp, tp = lax.axis_index("sp"), lax.axis_index("tp")
    z, x = sp // 2, sp % 2
    heads = state.shape[0]
    to_x = {"sp": z * 2 + (1 - x), "tp": tp}

    def later(i):
        return {"sp": ((z + i) % planes) * 2 + x, "tp": tp}

    def plane_of(i):
        return (z + planes - i) % planes

    def move(kind, i, ref, device):
        return pltpu.make_async_remote_copy(
            src_ref=ref, dst_ref=ref, send_sem=ssem.at[kind, i], recv_sem=rsem.at[kind, i],
            device_id=device, device_id_type=pl.DeviceIdType.MESH,
        )

    own = [
        pltpu.make_async_copy(state, gs.at[z, x], lsem.at[0]),
        pltpu.make_async_copy(totals, gt.at[z, x], lsem.at[1]),
    ]
    for copy in own:
        copy.start()
    greet([to_x] + [later(i) for i in range(1, planes)])
    for copy in own:
        copy.wait()
    for i in range(1, planes):
        move(0, i, gs.at[z, x], later(i)).start()
        move(1, i, gt.at[z, x], later(i)).start()
    for i in range(planes):
        p = plane_of(i)
        if i > 0:
            move(0, i, gs.at[p, x], to_x).wait_recv()
            move(1, i, gt.at[p, x], to_x).wait_recv()
        move(2, i, gs.at[p, x], to_x).start()
        move(3, i, gt.at[p, x], to_x).start()
    for i in range(planes):
        p = plane_of(i)
        move(2, i, gs.at[p, 1 - x], to_x).wait_recv()
        move(3, i, gt.at[p, 1 - x], to_x).wait_recv()
    running = jnp.zeros((8, HEAD_DIM), jnp.float32)
    sums = [jnp.zeros((HEAD_DIM, HEAD_DIM), jnp.float32) for _ in range(heads)]
    for s in reversed(range(2 * planes)):
        earlier = s < sp
        factor = jnp.where(earlier, jnp.exp(running), 0.0)
        running = running + jnp.where(earlier, gt[s // 2, s % 2], 0.0)
        for h in range(heads):
            sums[h] = sums[h] + factor[h : h + 1, :] * gs[s // 2, s % 2, h].astype(jnp.float32)
    for h in range(heads):
        entering[h] = sums[h].astype(jnp.bfloat16)
    for i in range(planes):
        p = plane_of(i)
        if i > 0:
            move(0, i, gs.at[z, x], to_x).wait_send()
            move(1, i, gt.at[z, x], to_x).wait_send()
        move(2, i, gs.at[p, x], to_x).wait_send()
        move(3, i, gt.at[p, x], to_x).wait_send()


def mix_kernel(part, out, from_core, held, from_y, ssem, rsem):
    sp, tp = lax.axis_index("sp"), lax.axis_index("tp")
    y, c = tp // 2, tp % 2
    to_core = {"sp": sp, "tp": y * 2 + (1 - c)}
    to_y = {"sp": sp, "tp": (1 - y) * 2 + c}

    def move(i, src, dst, device):
        return pltpu.make_async_remote_copy(
            src_ref=src, dst_ref=dst, send_sem=ssem.at[i], recv_sem=rsem.at[i],
            device_id=device, device_id_type=pl.DeviceIdType.MESH,
        )

    greet([to_core, to_y])
    far = move(0, part.at[1 - y, 1 - c], from_core.at[0], to_core)
    near = move(1, part.at[y, 1 - c], from_core.at[1], to_core)
    far.start()
    near.start()
    far.wait_recv()
    held[0] = (
        part[1 - y, c].astype(jnp.float32) + from_core[0].astype(jnp.float32)
    ).astype(jnp.bfloat16)
    across = move(2, held.at[0], from_y, to_y)
    across.start()
    near.wait_recv()
    mine = part[y, c].astype(jnp.float32) + from_core[1].astype(jnp.float32)
    across.wait_recv()
    out[...] = mine + from_y[...].astype(jnp.float32)
    far.wait_send()
    near.wait_send()
    across.wait_send()


def retention(query_rows, key_rows, value_rows, gate_rows, log_decay, head_gain):
    length, local_heads = log_decay.shape
    width = query_rows.shape[1]
    sp_count, mine = lax.axis_size("sp"), lax.axis_index("sp")
    positions = (mine * length + jnp.arange(length, dtype=jnp.int32)).astype(jnp.float32)
    angles = rotary_angles(positions, HEAD_DIM)
    cosine, sine = jnp.cos(angles), jnp.sin(angles)
    cosine = jnp.concatenate([cosine, cosine], axis=1)
    sine = jnp.concatenate([-sine, sine], axis=1)
    cumulative = jnp.cumsum(log_decay, axis=0)
    rows_spec = pl.BlockSpec((length, HEAD_DIM), lambda h: (0, h))
    table_spec = pl.BlockSpec((length, HEAD_DIM), lambda h: (0, 0))
    retained, qdec, state = pl.pallas_call(
        retention_kernel,
        grid=(local_heads,),
        out_shape=(
            jax.ShapeDtypeStruct((length, width), jnp.float32),
            jax.ShapeDtypeStruct((length, width), jnp.bfloat16),
            jax.ShapeDtypeStruct((local_heads, HEAD_DIM + 8, HEAD_DIM), jnp.float32),
        ),
        in_specs=[
            rows_spec,
            rows_spec,
            rows_spec,
            table_spec,
            table_spec,
            pl.BlockSpec((length, local_heads), lambda h: (0, 0)),
            pl.BlockSpec((1, 1, length), lambda h: (h, 0, 0)),
        ],
        out_specs=(
            rows_spec,
            rows_spec,
            pl.BlockSpec((1, HEAD_DIM + 8, HEAD_DIM), lambda h: (h, 0, 0)),
        ),
    )(query_rows, key_rows, value_rows, cosine, sine, cumulative, cumulative.T[:, None, :])
    if sp_count % 2 == 0 and local_heads <= 8 and sp_count <= 16:
        totals = jnp.broadcast_to(state[:, HEAD_DIM, :1], (local_heads, HEAD_DIM))
        totals = jnp.pad(totals, ((0, 8 - local_heads), (0, 0)))
        planes = sp_count // 2
        block = (local_heads, HEAD_DIM, HEAD_DIM)
        entering = pl.pallas_call(
            functools.partial(state_kernel, planes),
            out_shape=jax.ShapeDtypeStruct(block, jnp.bfloat16),
            in_specs=[pl.BlockSpec(memory_space=pltpu.VMEM)] * 2,
            out_specs=pl.BlockSpec(memory_space=pltpu.VMEM),
            scratch_shapes=[
                pltpu.VMEM((planes, 2) + block, jnp.bfloat16),
                pltpu.VMEM((planes, 2, 8, HEAD_DIM), jnp.float32),
                pltpu.SemaphoreType.DMA((4, planes)),
                pltpu.SemaphoreType.DMA((4, planes)),
                pltpu.SemaphoreType.DMA((2,)),
            ],
            compiler_params=pltpu.CompilerParams(collective_id=1, has_side_effects=True),
        )(state[:, :HEAD_DIM, :].astype(jnp.bfloat16), totals)
    else:
        pieces = lax.all_gather(state, "sp")
        totals = pieces[:, :, HEAD_DIM, 0]
        index = jnp.arange(sp_count, dtype=jnp.int32)
        between = (index[None, :] > index[:, None]) & (index[None, :] < mine)
        gap = jnp.sum(jnp.where(between[:, :, None], totals[None], 0.0), axis=1)
        factor = jnp.where((index < mine)[:, None], jnp.exp(gap), 0.0)
        entering = jnp.sum(factor[:, :, None, None] * pieces[:, :, :HEAD_DIM, :], axis=0)
    return pl.pallas_call(
        norm_kernel,
        grid=(local_heads,),
        out_shape=jax.ShapeDtypeStruct((length, width), jnp.bfloat16),
        in_specs=[
            rows_spec,
            rows_spec,
            pl.BlockSpec((1, HEAD_DIM, HEAD_DIM), lambda h: (h, 0, 0)),
            pl.BlockSpec((1, HEAD_DIM), lambda h: (0, h)),
            rows_spec,
        ],
        out_specs=rows_spec,
    )(retained, qdec, entering, head_gain[None, :], gate_rows)


Z_A, Z_B, X_A2, Y_B2, Y_A3, Y_A4, X_B3, X_B4, C_A, C_B, C_P, Y_A, X_B, X_A, Y_B, RZ_A, RZ_B = range(17)


def experts_kernel(
    planes, x0, x1, upd, wg, wu, wd, out,
    g0, g1, pm, pc, pr, a0, a1, r10, r11, b0, b1, r20, r21, d0, d1, z0, z1,
    ssem, rsem, lsem,
):
    sp, tp = lax.axis_index("sp"), lax.axis_index("tp")
    sp_count = 2 * planes
    z, x = sp // 2, sp % 2
    y, c = tp // 2, tp % 2
    half = x1.shape[1]
    rows = x1.shape[0]
    f32, bf16 = jnp.float32, jnp.bfloat16
    to_core = {"sp": sp, "tp": y * 2 + (1 - c)}
    to_y = {"sp": sp, "tp": (1 - y) * 2 + c}
    to_x = {"sp": z * 2 + (1 - x), "tp": tp}

    def plane_of(i):
        return (z + planes - i) % planes

    def to_z(i):
        return {"sp": plane_of(i) * 2 + x, "tp": tp}

    def from_z(i):
        return {"sp": ((z + i) % planes) * 2 + x, "tp": tp}

    def move(kind, i, src, dst, device):
        return pltpu.make_async_remote_copy(
            src_ref=src, dst_ref=dst, send_sem=ssem.at[kind, i], recv_sem=rsem.at[kind, i],
            device_id=device, device_id_type=pl.DeviceIdType.MESH,
        )

    def send(kind, i, src, dst, device):
        move(kind, i, src, dst, device).start()

    def arrived(kind, i, dst):
        move(kind, i, dst, dst, to_core).wait_recv()

    def left(kind, i, src):
        move(kind, i, src, src, to_core).wait_send()

    barrier = pltpu.get_barrier_semaphore()
    for device in [to_core, to_y, to_x] + [to_z(i) for i in range(1, planes)]:
        pl.semaphore_signal(barrier, inc=1, device_id=device, device_id_type=pl.DeviceIdType.MESH)
    pl.semaphore_wait(barrier, 2 + planes)

    here = x * 2 + y
    other_x = (1 - x) * 2 + y
    other_y = x * 2 + (1 - y)
    other_xy = (1 - x) * 2 + (1 - y)
    own0 = pltpu.make_async_copy(x0, g0.at[c, z, here], lsem.at[0])
    own1 = pltpu.make_async_copy(x1, g1.at[c, z, here], lsem.at[1])
    own0.start()
    own1.start()
    own0.wait()
    own1.wait()
    for i in range(1, planes):
        send(Z_A, i, g0.at[c, z, here], g0.at[c, z, here], from_z(i))
        send(Z_B, i, g1.at[c, z, here], g1.at[c, z, here], from_z(i))

    def compute(i, core):
        p = plane_of(i)
        left_rows = g0[core, p].reshape(4 * rows, half + 128)
        right_rows = g1[core, p].reshape(4 * rows, half)
        tail = left_rows[:, half:].astype(f32)
        left_rows = left_rows[:, :half]
        lane = lax.broadcasted_iota(jnp.int32, tail.shape, 1)
        weight = jnp.sum(
            jnp.where((lane == sp) | (lane == sp + sp_count), tail, 0.0), axis=1, keepdims=True
        )

        def product(w):
            return jnp.dot(left_rows, w[:half, :], preferred_element_type=f32) + jnp.dot(
                right_rows, w[half:, :], preferred_element_type=f32
            )

        gate = jnp.minimum(product(wg), clamp_limit)
        up = jnp.clip(product(wu), -clamp_limit, clamp_limit)
        act = ((up + 1.0) * (gate / (1.0 + jnp.exp(-swish_alpha * gate)))).astype(bf16)
        return (jnp.dot(act, wd[...], preferred_element_type=f32) * weight).astype(bf16)

    def step(i, carry):
        @pl.when((i >= 1) & (i < planes + 1))
        def _():
            j = i - 1
            p = plane_of(j)
            arrived(Y_A3, j, g0.at[c, p, other_y])
            arrived(Y_A4, j, g0.at[c, p, other_xy])
            arrived(X_B3, j, g1.at[c, p, other_x])
            arrived(X_B4, j, g1.at[c, p, other_xy])
            send(C_A, j, g0.at[c, p], g0.at[c, p], to_core)
            send(C_B, j, g1.at[c, p], g1.at[c, p], to_core)

        @pl.when(i < planes)
        def _():
            p = plane_of(i)

            @pl.when(i > 0)
            def _():
                arrived(Z_A, i, g0.at[c, p, here])
                arrived(Z_B, i, g1.at[c, p, here])

            send(X_A2, i, g0.at[c, p, here], g0.at[c, p, here], to_x)
            send(Y_B2, i, g1.at[c, p, here], g1.at[c, p, here], to_y)
            send(Y_A3, i, g0.at[c, p, here], g0.at[c, p, here], to_y)
            send(X_B3, i, g1.at[c, p, here], g1.at[c, p, here], to_x)
            arrived(X_A2, i, g0.at[c, p, other_x])
            send(Y_A4, i, g0.at[c, p, other_x], g0.at[c, p, other_x], to_y)
            arrived(Y_B2, i, g1.at[c, p, other_y])
            send(X_B4, i, g1.at[c, p, other_y], g1.at[c, p, other_y], to_x)

        @pl.when((i >= 2) & (i < planes + 2))
        def _():
            j = i - 2
            arrived(C_P, j, pr.at[j])
            for q in range(4):
                part = pl.ds(q * rows, rows)
                total = (pm[j, part, :].astype(f32) + pr[j, part, :].astype(f32)).astype(bf16)
                a0[j, q % 2, q // 2] = total[:, :half]
                a1[j, q // 2, q % 2] = total[:, half:]
            send(Y_A, j, a0.at[j, 1 - y], r10.at[j], to_y)
            send(X_B, j, a1.at[j, 1 - x], r11.at[j], to_x)

        @pl.when((i >= 3) & (i < planes + 3))
        def _():
            j = i - 3
            arrived(Y_A, j, r10.at[j])
            b0[j] = (a0[j, y].astype(f32) + r10[j].astype(f32)).astype(bf16)
            send(X_A, j, b0.at[j, 1 - x], r20.at[j], to_x)
            arrived(X_B, j, r11.at[j])
            b1[j] = (a1[j, x].astype(f32) + r11[j].astype(f32)).astype(bf16)
            send(Y_B, j, b1.at[j, 1 - y], r21.at[j], to_y)

        @pl.when((i >= 4) & (i < planes + 4))
        def _():
            j = i - 4
            arrived(X_A, j, r20.at[j])
            d0[j] = (b0[j, x].astype(f32) + r20[j].astype(f32)).astype(bf16)
            arrived(Y_B, j, r21.at[j])
            d1[j] = (b1[j, y].astype(f32) + r21[j].astype(f32)).astype(bf16)

            @pl.when(j > 0)
            def _():
                send(RZ_A, j, d0.at[j], z0.at[j], to_z(j))
                send(RZ_B, j, d1.at[j], z1.at[j], to_z(j))

        @pl.when((i >= 1) & (i < planes + 1))
        def _():
            j = i - 1
            p = plane_of(j)
            arrived(C_A, j, g0.at[1 - c, p])
            arrived(C_B, j, g1.at[1 - c, p])

            def tile(turn, carry):
                @pl.when(turn == 0)
                def _():
                    pc[j] = compute(j, 1 - c)
                    send(C_P, j, pc.at[j], pr.at[j], to_core)

                @pl.when(turn == 1)
                def _():
                    pm[j] = compute(j, c)

                return carry

            lax.fori_loop(0, 2, tile, 0)

        return carry

    lax.fori_loop(0, planes + 4, step, 0)
    low, high = upd[:, :half], upd[:, half:]
    low = low + d0[0].astype(f32)
    high = high + d1[0].astype(f32)
    for i in range(1, planes):
        arrived(RZ_A, i, z0.at[i])
        low = low + z0[i].astype(f32)
        arrived(RZ_B, i, z1.at[i])
        high = high + z1[i].astype(f32)
    out[:, :half] = low.astype(bf16)
    out[:, half:] = high.astype(bf16)

    def drain(i, carry):
        p = plane_of(i)

        @pl.when(i > 0)
        def _():
            left(Z_A, i, g0.at[c, z, here])
            left(Z_B, i, g1.at[c, z, here])
            left(RZ_A, i, d0.at[i])
            left(RZ_B, i, d1.at[i])

        left(X_A2, i, g0.at[c, p, here])
        left(Y_B2, i, g1.at[c, p, here])
        left(Y_A3, i, g0.at[c, p, here])
        left(X_B3, i, g1.at[c, p, here])
        left(Y_A4, i, g0.at[c, p, other_x])
        left(X_B4, i, g1.at[c, p, other_y])
        left(C_A, i, g0.at[c, p])
        left(C_B, i, g1.at[c, p])
        left(C_P, i, pc.at[i])
        left(Y_A, i, a0.at[i, 1 - y])
        left(X_B, i, a1.at[i, 1 - x])
        left(X_A, i, b0.at[i, 1 - x])
        left(Y_B, i, b1.at[i, 1 - y])
        return carry

    lax.fori_loop(0, planes, drain, 0)


def dense_experts(updated, ffn_in, own_routes, route_weights, gate_part, up_part, down_part):
    sp_count, mine = lax.axis_size("sp"), lax.axis_index("sp")
    width = ffn_in.shape[1]
    chosen = own_routes[:, :, None] == jnp.arange(sp_count, dtype=jnp.int32)[None, None, :]
    shares = jnp.sum(jnp.where(chosen, route_weights[:, :, None], 0.0), axis=1)
    coarse = shares.astype(jnp.bfloat16)
    fine = (shares - coarse.astype(jnp.float32)).astype(jnp.bfloat16)
    spare = jnp.zeros((ffn_in.shape[0], 128 - 2 * sp_count), jnp.bfloat16)
    half = width // 2
    first = jnp.concatenate([ffn_in[:, :half], coarse, fine, spare], axis=1)
    second = ffn_in[:, half:]
    rows = ffn_in.shape[0]
    planes = sp_count // 2
    bf16 = jnp.bfloat16
    whole = pl.BlockSpec(memory_space=pltpu.VMEM)
    return pl.pallas_call(
        functools.partial(experts_kernel, planes),
        out_shape=jax.ShapeDtypeStruct((rows, width), bf16),
        in_specs=[whole] * 6,
        out_specs=whole,
        scratch_shapes=[
            pltpu.VMEM((2, planes, 4, rows, half + 128), bf16),
            pltpu.VMEM((2, planes, 4, rows, half), bf16),
            pltpu.VMEM((planes, 4 * rows, width), bf16),
            pltpu.VMEM((planes, 4 * rows, width), bf16),
            pltpu.VMEM((planes, 4 * rows, width), bf16),
            pltpu.VMEM((planes, 2, 2, rows, half), bf16),
            pltpu.VMEM((planes, 2, 2, rows, half), bf16),
            pltpu.VMEM((planes, 2, rows, half), bf16),
            pltpu.VMEM((planes, 2, rows, half), bf16),
            pltpu.VMEM((planes, 2, rows, half), bf16),
            pltpu.VMEM((planes, 2, rows, half), bf16),
            pltpu.VMEM((planes, rows, half), bf16),
            pltpu.VMEM((planes, rows, half), bf16),
            pltpu.VMEM((planes, rows, half), bf16),
            pltpu.VMEM((planes, rows, half), bf16),
            pltpu.VMEM((planes, rows, half), bf16),
            pltpu.VMEM((planes, rows, half), bf16),
            pltpu.SemaphoreType.DMA((17, planes)),
            pltpu.SemaphoreType.DMA((17, planes)),
            pltpu.SemaphoreType.DMA((2,)),
        ],
        compiler_params=pltpu.CompilerParams(
            collective_id=0, has_side_effects=True, vmem_limit_bytes=63 * 1024 * 1024
        ),
    )(first, second, updated, gate_part, up_part, down_part)


def body(
    query_rows,
    key_rows,
    value_rows,
    gate_rows,
    log_decay,
    head_gain,
    out_weight,
    residual,
    ffn_gain,
    gate_weight,
    up_weight,
    down_weight,
    routes,
    route_weights,
):
    tok_count = query_rows.shape[0]
    local_heads = log_decay.shape[1]
    sp_count = lax.axis_size("sp")
    tp_count = lax.axis_size("tp")
    model_width = residual.shape[1]
    rows_own = tok_count // tp_count
    capacity = max(2, 3 * rows_own * TOPK // (2 * sp_count))
    hidden = retention(query_rows, key_rows, value_rows, gate_rows, log_decay, head_gain)
    mixed = jnp.dot(hidden, out_weight, preferred_element_type=jnp.float32).astype(jnp.bfloat16)
    if tp_count == 4 and sp_count <= 16:
        mixed_sum = pl.pallas_call(
            mix_kernel,
            out_shape=jax.ShapeDtypeStruct((rows_own, model_width), jnp.float32),
            in_specs=[pl.BlockSpec(memory_space=pltpu.VMEM)],
            out_specs=pl.BlockSpec(memory_space=pltpu.VMEM),
            scratch_shapes=[
                pltpu.VMEM((2, rows_own, model_width), jnp.bfloat16),
                pltpu.VMEM((2, rows_own, model_width), jnp.bfloat16),
                pltpu.VMEM((rows_own, model_width), jnp.bfloat16),
                pltpu.SemaphoreType.DMA((3,)),
                pltpu.SemaphoreType.DMA((3,)),
            ],
            compiler_params=pltpu.CompilerParams(collective_id=2, has_side_effects=True),
        )(mixed.reshape(2, 2, rows_own, model_width))
    else:
        mixed_sum = lax.psum_scatter(mixed, "tp", scatter_dimension=0, tiled=True).astype(
            jnp.float32
        )
    updated = residual.astype(jnp.float32) + mixed_sum
    ffn_in = square_norm(updated, ffn_gain)
    tp_index = lax.axis_index("tp")
    own_routes = lax.dynamic_slice_in_dim(routes, tp_index * rows_own, rows_own, 0)
    if rows_own < 2 * capacity and 2 * sp_count <= 128 and sp_count % 2 == 0 and tp_count == 4:
        return dense_experts(
            updated, ffn_in, own_routes, route_weights, gate_weight[0], up_weight[0], down_weight[0]
        )
    own_experts, own_ranks = slot_ranks(own_routes, sp_count)
    home_slot = own_experts * capacity + own_ranks
    gate_part = gate_weight[0]
    up_part = up_weight[0]
    down_part = down_weight[0]
    empty_row = jnp.zeros((1, model_width), jnp.bfloat16)
    source_row = (
        jnp.full((sp_count * capacity,), rows_own, jnp.int32)
        .at[home_slot]
        .set(jnp.arange(rows_own * TOPK, dtype=jnp.int32) // TOPK)
    )
    padded = jnp.concatenate([ffn_in, empty_row], axis=0)
    outgoing = padded[source_row].reshape(sp_count, capacity, model_width)
    arrived = lax.all_to_all(outgoing, "sp", split_axis=0, concat_axis=0, tiled=True)
    fanned = lax.all_gather(arrived[None], "tp", axis=0, tiled=True)
    activity = expert_rows(fanned.reshape(-1, model_width), gate_part, up_part)
    partial_out = jnp.dot(activity, down_part, preferred_element_type=jnp.float32).reshape(
        tp_count, sp_count, capacity, model_width
    )
    summed = (
        lax.psum_scatter(partial_out.astype(jnp.bfloat16), "tp", scatter_dimension=0, tiled=True)
        .astype(jnp.float32)
        .reshape(sp_count, capacity, model_width)
    )
    returned = lax.all_to_all(
        summed.astype(jnp.bfloat16), "sp", split_axis=0, concat_axis=0, tiled=True
    )
    picked = returned.reshape(sp_count * capacity, model_width)[home_slot].reshape(
        rows_own, TOPK, model_width
    )
    expert_sum = jnp.sum(route_weights[:, :, None] * picked.astype(jnp.float32), axis=1)
    return (updated + expert_sum).astype(jnp.bfloat16)


def solution(mesh):
    return jax.shard_map(
        body,
        mesh=mesh,
        in_specs=(
            P("sp", "tp"),
            P("sp", "tp"),
            P("sp", "tp"),
            P("sp", "tp"),
            P("sp", "tp"),
            P("tp"),
            P("tp", None),
            P(("sp", "tp"), None),
            P(),
            P("sp", None, "tp"),
            P("sp", None, "tp"),
            P("sp", "tp", None),
            P("sp", None),
            P(("sp", "tp"), None),
        ),
        out_specs=P(("sp", "tp"), None),
        check_vma=False,
    )
```
